128 devices in a mesh: sp: 32 (over z, y, core), tp: 4 (over x).
Axes of the slice: x: 4, y: 4, z: 4, core: 2. Of those that a mesh axis runs over, the one named last changes fastest.
Arguments:
- tokens: bfloat16 [16384, 2048], P(('sp', 'tp')), may hold values from -6 to 6
- norm_gain: float32 [2048], replicated, may hold values from 0.1 to 1.9
- query_weight: bfloat16 [2048, 2048], P('sp', 'tp'), may hold values from -0.125 to 0.125
- key_weight: bfloat16 [2048, 2048], P('sp', 'tp'), may hold values from -0.125 to 0.125
- value_weight: bfloat16 [2048, 4096], P('sp', 'tp'), may hold values from -0.125 to 0.125
- retain_gate: bfloat16 [2048, 4096], P('sp', 'tp'), may hold values from -0.125 to 0.125
- unit_value: bfloat16 [2048, 2048], P('sp', 'tp'), may hold values from -0.125 to 0.125
- unit_gate: bfloat16 [2048, 2048], P('sp', 'tp'), may hold values from -0.125 to 0.125
- convolve_gate: bfloat16 [2048, 2048], P('sp', 'tp'), may hold values from -0.125 to 0.125
- filter_taps: float32 [31, 2048], replicated, may hold values from -1 to 1
- layer_gain: float32 [2048], replicated, may hold values from 0.1 to 1.9
- layer_shift: float32 [2048], replicated, may hold values from -3 to 3
- retain_output: bfloat16 [2048, 4096], P('sp', 'tp'), may hold values from -0.09375 to 0.09375
- convolve_output: bfloat16 [2048, 2048], P('sp', 'tp'), may hold values from -0.125 to 0.125
Outputs:
- mixed: bfloat16 [16384, 2048], P(('sp', 'tp'))
The draws below stay inside these ranges and needn't reach their ends.
All inputs are finite; a program needn't handle non-finite values.
Results may differ from the reference program's by a relative error of at most 0.018.
Values may be sent and summed in bfloat16 or wider, within the bound.
A program may use at most 128 MiB of HBM per device.

```python
import jax
import jax.numpy as jnp
from jax import lax

D = 2048
HEADS = 8
KEY = 256
VAL = 512
CONV = 2048
GROUP = 512
KW = 31
TOK_DEV = 512
QK = 2048
VW = 4096
SEQ = 16384


def steps_of(stream_key, shape, cuts, smallest, top_value):
    gain, own = 1.0, jax.random.fold_in(stream_key, 6)
    for dim, shards_of in cuts:
        draws = jnp.exp(jax.random.uniform(jax.random.fold_in(own, dim), (shards_of,), jnp.float32, smallest / len(cuts), top_value / len(cuts)))
        gain = gain * jnp.repeat(draws, shape[dim] // shards_of).reshape([-1 if axis == dim else 1 for axis in range(len(shape))])
    return gain


def centred(own_key, extent, scale, most, shards=(), kind=jnp.bfloat16):
    drawn = jax.random.normal(own_key, extent, jnp.float32) * scale
    if len(shards) > 0:
        drawn = steps_of(own_key, extent, shards, -0.22, 0.18) * drawn
    return jnp.clip(drawn, min=-most, max=most).astype(kind)


def setup_inputs(seed: int = 0) -> dict:
    keys = jax.random.split(jax.random.key(seed), 15)
    return {
        "tokens": centred(keys[0], (SEQ, D), 1.0, 6.0, ((0, 128),)),
        "norm_gain": jnp.clip(1.0 + 0.18 * jax.random.normal(keys[1], (D,), jnp.float32), 0.1, 1.9),
        "query_weight": centred(keys[2], (D, QK), D ** -0.5, 0.125, ((0, 32), (1, 4))),
        "key_weight": centred(keys[3], (D, QK), D ** -0.5, 0.125, ((0, 32), (1, 4))),
        "value_weight": centred(keys[4], (D, VW), D ** -0.5, 0.125, ((0, 32), (1, 4))),
        "retain_gate": centred(keys[5], (D, VW), D ** -0.5, 0.125, ((0, 32), (1, 4))),
        "unit_value": centred(keys[6], (D, CONV), D ** -0.5, 0.125, ((0, 32), (1, 4))),
        "unit_gate": centred(keys[7], (D, CONV), D ** -0.5, 0.125, ((0, 32), (1, 4))),
        "convolve_gate": centred(keys[8], (D, CONV), D ** -0.5, 0.125, ((0, 32), (1, 4))),
        "filter_taps": centred(keys[9], (KW, CONV), KW ** -0.5, 1.0, (), jnp.float32),
        "layer_gain": jnp.clip(1.0 + 0.18 * jax.random.normal(keys[10], (CONV,), jnp.float32), 0.1, 1.9),
        "layer_shift": centred(keys[11], (CONV,), 0.5, 3.0, (), jnp.float32),
        "retain_output": centred(keys[12], (D, VW), VW ** -0.5, 0.09375, ((0, 32), (1, 4))),
        "convolve_output": centred(keys[13], (D, CONV), CONV ** -0.5, 0.125, ((0, 32), (1, 4))),
    }


rms_eps = 1e-06
group_eps = 1.0
layer_eps = 0.001
rope_base = 10000.0
highest = lax.Precision.HIGHEST

def rms_normalize(tokens, norm_gain):
    widened = tokens.astype(jnp.float32)
    scaled = widened * lax.rsqrt(lax.optimization_barrier(jnp.mean(widened * widened, axis=-1, keepdims=True)) + rms_eps)
    return (scaled * norm_gain).astype(jnp.bfloat16)

def widen(narrow_value):
    return lax.optimization_barrier(narrow_value.astype(jnp.bfloat16)).astype(jnp.float32)

def rotate(vectors, positions):
    half_width = vectors.shape[-1] // 2
    frequency = rope_base ** (-jnp.arange(half_width, dtype=jnp.float32) / half_width)
    angles = positions.astype(jnp.float32)[:, None] * frequency
    cosine = jnp.cos(angles)[:, None, :]
    sine_part = jnp.sin(angles)[:, None, :]
    front_half = vectors[..., :half_width]
    back_half = vectors[..., half_width:]
    return jnp.concatenate([front_half * cosine - back_half * sine_part, front_half * sine_part + back_half * cosine], axis=-1)

def prepare(queries, key_rows, values, positions):
    row_count = queries.shape[0]
    rotated_query = widen(rotate(queries.astype(jnp.float32).reshape(row_count, -1, KEY), positions))
    rotated_keys = widen(rotate(key_rows.astype(jnp.float32).reshape(row_count, -1, KEY), positions) * KEY ** (-0.5))
    value_heads = values.astype(jnp.float32).reshape(row_count, -1, VAL)
    return (rotated_query, rotated_keys, value_heads)

def decay_logs(first_head, head_total, all_heads, seq_length):
    ratio = (first_head + jnp.arange(head_total)).astype(jnp.float32) / (all_heads - 1)
    return (jnp.log(0.05) + ratio * jnp.log(18.0)) / seq_length

def local_parts(queries, key_rows, values, log_decay):
    row_count = queries.shape[0]
    indices = jnp.arange(row_count, dtype=jnp.float32)
    offsets = indices[:, None] - indices[None, :]
    causal = offsets >= 0
    weight = jnp.where(causal[None], jnp.exp(log_decay[:, None, None] * jnp.where(causal, offsets, 0.0)[None]), 0.0)
    scores = widen(jnp.einsum('ihd,jhd->hij', queries, key_rows) * weight)
    within = jnp.einsum('hij,jhe->ihe', scores, values)
    trailing = jnp.exp(log_decay[None, :] * (row_count - 1.0 - indices)[:, None])
    weighted = widen(key_rows * trailing[:, :, None])
    contribution = jnp.einsum('jhd,jhe->hde', weighted, values)
    return (within, contribution)

def cross_part(queries, carry_state, log_decay):
    row_count = queries.shape[0]
    indices = jnp.arange(row_count, dtype=jnp.float32)
    leading = jnp.exp(log_decay[None, :] * (indices + 1.0)[:, None])
    return jnp.einsum('ihd,hde->ihe', queries, carry_state, precision=highest) * leading[:, :, None]

def retain_finish(raw, switch):
    average = lax.optimization_barrier(jnp.mean(raw, axis=-1, keepdims=True))
    spread = lax.optimization_barrier(jnp.mean(jnp.square(raw - average), axis=-1, keepdims=True))
    normalized = ((raw - average) * lax.rsqrt(spread + group_eps)).reshape(raw.shape[0], -1)
    return (normalized * jax.nn.silu(switch.astype(jnp.float32))).astype(jnp.bfloat16)

def convolve_branch(gated_input, before, tap_slice, gain_slice, shift_slice, switch):
    padded = jnp.concatenate([before, gated_input], axis=0)
    row_count = gated_input.shape[0]
    summed = jnp.zeros(gated_input.shape, jnp.float32)
    for tap_index in range(tap_slice.shape[0]):
        summed = summed + padded[tap_index:tap_index + row_count].astype(jnp.float32) * tap_slice[tap_index]
    grouped = summed.reshape(row_count, -1, GROUP)
    average = lax.optimization_barrier(jnp.mean(grouped, axis=-1, keepdims=True))
    spread = lax.optimization_barrier(jnp.mean(jnp.square(grouped - average), axis=-1, keepdims=True))
    normalized = ((grouped - average) * lax.rsqrt(spread + layer_eps)).reshape(row_count, -1)
    normalized = normalized * gain_slice + shift_slice
    return (jax.nn.silu(normalized) * jax.nn.silu(switch.astype(jnp.float32))).astype(jnp.bfloat16)

def contract(hidden, matrix):
    return lax.dot_general(hidden, matrix, (((1,), (1,)), ((), ())), preferred_element_type=jnp.float32)

def reference(tokens, norm_gain, query_weight, key_weight, value_weight, retain_gate, unit_value, unit_gate, convolve_gate, filter_taps, layer_gain, layer_shift, retain_output, convolve_output):
    seq_total = tokens.shape[0]
    normed = rms_normalize(tokens, norm_gain)

    def project(matrix):
        return jnp.dot(normed, matrix, preferred_element_type=jnp.float32).astype(jnp.bfloat16)
    queries = project(query_weight)
    key_rows = project(key_weight)
    values = project(value_weight)
    retain_switch = project(retain_gate)
    glu_value = project(unit_value)
    glu_switch = project(unit_gate)
    convolve_switch = project(convolve_gate)
    positions = jnp.arange(seq_total, dtype=jnp.int32)
    rotated_query, rotated_keys, value_heads = prepare(queries, key_rows, values, positions)
    log_decay = decay_logs(0, HEADS, HEADS, seq_total)
    totals = jnp.exp(log_decay * TOK_DEV)
    blocks = seq_total // TOK_DEV

    def advance(carry_state, block):
        block_query, block_keys, block_values = block
        within, contribution = local_parts(block_query, block_keys, block_values, log_decay)
        result = within + cross_part(block_query, carry_state, log_decay)
        return (carry_state * totals[:, None, None] + contribution, result)
    start_state = jnp.zeros((HEADS, KEY, VAL), jnp.float32)
    final_state, outputs = lax.scan(advance, start_state, (rotated_query.reshape(blocks, TOK_DEV, HEADS, KEY), rotated_keys.reshape(blocks, TOK_DEV, HEADS, KEY), value_heads.reshape(blocks, TOK_DEV, HEADS, VAL)))
    raw = outputs.reshape(seq_total, HEADS, VAL)
    retain_hidden = retain_finish(raw, retain_switch)
    gated_input = (glu_value.astype(jnp.float32) * jax.nn.sigmoid(glu_switch.astype(jnp.float32))).astype(jnp.bfloat16)
    before = jnp.zeros((KW - 1, CONV), jnp.bfloat16)
    convolve_hidden = convolve_branch(gated_input, before, filter_taps, layer_gain, layer_shift, convolve_switch)
    summed = contract(retain_hidden, retain_output) + contract(convolve_hidden, convolve_output)
    return summed.astype(jnp.bfloat16)
```

```python
import functools

import jax
import jax.numpy as jnp
from jax import lax
from jax.experimental import pallas as pl
from jax.experimental.pallas import tpu as pltpu
from jax.sharding import PartitionSpec as P

MESH = pl.DeviceIdType.MESH
KEY = 256
VAL = 512
GROUP = 512
KW = 31
rms_eps = 1e-06
group_eps = 1.0
layer_eps = 0.001
rope_base = 10000.0
HOPS = (0, 3, 1, 2)


def body(
    tok,
    gain,
    wq,
    wk,
    wv,
    wrg,
    wuv,
    wug,
    wcg,
    wro,
    wco,
    p0,
    p1,
    p2,
    w3,
    W,
    N,
    tokv,
    gainv,
    PV,
    lsem,
    wss,
    wrs,
    nss,
    nrs,
    osem,
):
    sp = lax.axis_index("sp")
    x = lax.axis_index("tp")
    c = sp % 2
    y = (sp // 2) % 4
    z = sp // 8

    def coords(k1, k2, cc):
        ky = k1 * (1 - cc) + k2 * cc
        kz = k2 * (1 - cc) + k1 * cc
        return (z + kz) % 4, (y + ky) % 4

    def device(k1, k2):
        zz, yy = coords(k1, k2, c)
        return ((zz * 4 + yy) * 2 + c, x)

    n1p, n1m, n2p, n2m = device(1, 0), device(3, 0), device(0, 1), device(0, 3)
    partner = ((z * 4 + y) * 2 + 1 - c, x)
    xp, xm = (sp, (x + 1) % 4), (sp, (x + 3) % 4)

    def block(g, k1, k2, lo=0, rows=64):
        zz, yy = coords(k1, k2, c)
        return W.at[g, zz, yy, c, pl.ds(lo, rows), :]

    def other(g, k1, k2):
        zz, yy = coords(k1, k2, 1 - c)
        return W.at[g, zz, yy, 1 - c]

    loads = []

    def load(src, dst, i):
        cp = pltpu.make_async_copy(src, dst, lsem.at[i])
        cp.start()
        loads.append(cp)

    load(tok, tokv, 0)
    load(gain, gainv, 1)
    own = lambda g, a, b: W.at[g, z, y, c, :, pl.ds(a, b)]
    load(wk, own(0, 0, 512), 2)
    load(wv, own(0, 512, 1024), 3)
    load(wq, own(1, 0, 512), 4)
    load(wuv, own(1, 512, 512), 5)
    load(wug, own(1, 1024, 512), 6)
    load(wrg, own(2, 0, 1024), 7)
    load(wcg, own(2, 1024, 512), 8)
    load(wro, own(3, 0, 1024), 9)
    load(wco, own(3, 1024, 512), 10)

    barrier = pltpu.get_barrier_semaphore()
    for dev in (n1p, n1m, n2p, n2m, partner, xp, xm):
        pl.semaphore_signal(barrier, inc=1, device_id=dev, device_id_type=MESH)
    for cp in loads[2:4]:
        cp.wait()
    pl.semaphore_wait(barrier, 7)

    sends = []

    def remote(ref, ss, rs, dev):
        return pltpu.make_async_remote_copy(
            src_ref=ref, dst_ref=ref, send_sem=ss, recv_sem=rs, device_id=dev, device_id_type=MESH
        )

    def wsend(ref, g, i, dev):
        cp = remote(ref, wss.at[g, i], wrs.at[g, i], dev)
        cp.start()
        sends.append(cp)

    def wwait(ref, g, i):
        remote(ref, wss.at[g, i], wrs.at[g, i], partner).wait_recv()

    def s1(g):
        wsend(block(g, 0, 0), g, 0, n1p)
        wsend(block(g, 0, 0), g, 1, n1m)

    def s2(g):
        wwait(block(g, 3, 0), g, 0)
        wsend(block(g, 3, 0, 0, 32), g, 2, n1p)
        wwait(block(g, 1, 0), g, 1)
        wsend(block(g, 1, 0, 32, 32), g, 3, n1m)

    def s3(g):
        for j in range(3):
            k = HOPS[j]
            wsend(block(g, k, 0), g, 4 + j, n2p)
            wsend(block(g, k, 0), g, 8 + j, n2m)
            wsend(block(g, k, 0), g, 20 + j, partner)

    def s3b(g):
        wwait(block(g, 2, 0, 0, 32), g, 2)
        wwait(block(g, 2, 0, 32, 32), g, 3)
        wsend(block(g, 2, 0), g, 7, n2p)
        wsend(block(g, 2, 0), g, 11, n2m)
        wsend(block(g, 2, 0), g, 23, partner)

    def s4(g, j):
        k = HOPS[j]
        wwait(block(g, k, 3), g, 4 + j)
        wsend(block(g, k, 3, 0, 32), g, 12 + j, n2p)
        wsend(block(g, k, 3), g, 24 + j, partner)
        wwait(block(g, k, 1), g, 8 + j)
        wsend(block(g, k, 1, 32, 32), g, 16 + j, n2m)
        wsend(block(g, k, 1), g, 28 + j, partner)

    def s5(g, j):
        k = HOPS[j]
        wwait(block(g, k, 2, 0, 32), g, 12 + j)
        wwait(block(g, k, 2, 32, 32), g, 16 + j)
        wsend(block(g, k, 2), g, 32 + j, partner)

    def s6(g):
        for j in range(4):
            for q, k2 in enumerate((0, 3, 1, 2)):
                wwait(other(g, HOPS[j], k2), g, 20 + 4 * q + j)

    s1(0)
    loads[0].wait()
    loads[1].wait()
    tk = tokv[...].astype(jnp.float32)
    scale = lax.rsqrt(jnp.mean(tk * tk, axis=-1, keepdims=True) + rms_eps)
    N[x] = (tk * scale * gainv[...]).astype(jnp.bfloat16)
    for cp in loads[4:]:
        cp.wait()
    s1(1)
    s2(0)

    def nsend(ref, i, dev):
        cp = remote(ref, nss.at[i], nrs.at[i], dev)
        cp.start()
        sends.append(cp)

    def nwait(ref, i):
        remote(ref, nss.at[i], nrs.at[i], partner).wait_recv()

    nsend(N.at[x], 0, xp)
    nsend(N.at[x], 1, xm)

    def project(g, n):
        cols = pl.ds(pl.multiple_of(n * 256, 256), 256)
        w = W[g, :, :, :, :, cols].reshape(2048, 256)
        lhs = N[...].reshape(512, 2048)
        PV[g, :, cols] = jnp.dot(lhs, w, preferred_element_type=jnp.float32).astype(jnp.bfloat16)

    outs = (p0, p1, p2)
    for g in range(4):
        s3(g)
        if g + 2 < 4:
            s1(g + 2)
        s3b(g)
        if g + 1 < 4:
            s2(g + 1)
        if g == 0:
            xl, xr = (x + 3) % 4, (x + 1) % 4
            nwait(N.at[xl], 0)
            nsend(N.at[xl, pl.ds(0, 64), :], 2, xp)
            nwait(N.at[xr], 1)
            nsend(N.at[xr, pl.ds(64, 64), :], 3, xm)
        for j in range(4):
            s4(g, j)
            if g > 0 and j < 3:

                def step(i, carry, g=g, j=j):
                    project(g - 1, j * 2 + i)
                    return carry

                lax.fori_loop(0, 2, step, 0)
        if g > 0:
            cp = pltpu.make_async_copy(PV.at[g - 1], outs[g - 1], osem.at[g - 1])
            cp.start()
            loads.append(cp)
        for j in range(4):
            s5(g, j)
        if g == 0:
            xf = (x + 2) % 4
            nwait(N.at[xf, pl.ds(0, 64), :], 2)
            nwait(N.at[xf, pl.ds(64, 64), :], 3)
        s6(g)
    cp = pltpu.make_async_copy(W.at[3], w3, osem.at[3])
    cp.start()
    cp.wait()
    for cp in loads[11:]:
        cp.wait()
    for cp in sends:
        cp.wait_send()


def gather_project(tokens, norm_gain, *ws):
    any_spec = pl.BlockSpec(memory_space=pl.ANY)
    bf = jnp.bfloat16
    return pl.pallas_call(
        body,
        out_shape=[jax.ShapeDtypeStruct((512, 1536), bf)] * 3
        + [jax.ShapeDtypeStruct((4, 4, 2, 64, 1536), bf)],
        in_specs=[any_spec] * 11,
        out_specs=[any_spec] * 4,
        scratch_shapes=[
            pltpu.VMEM((4, 4, 4, 2, 64, 1536), bf),
            pltpu.VMEM((4, 128, 2048), bf),
            pltpu.VMEM((128, 2048), bf),
            pltpu.VMEM((1, 2048), jnp.float32),
            pltpu.VMEM((3, 512, 1536), bf),
            pltpu.SemaphoreType.DMA((11,)),
            pltpu.SemaphoreType.DMA((4, 36)),
            pltpu.SemaphoreType.DMA((4, 36)),
            pltpu.SemaphoreType.DMA((4,)),
            pltpu.SemaphoreType.DMA((4,)),
            pltpu.SemaphoreType.DMA((4,)),
        ],
        compiler_params=pltpu.CompilerParams(
            collective_id=0, has_side_effects=True, vmem_limit_bytes=56 * 1024 * 1024
        ),
        name="gather_project",
    )(tokens, norm_gain, *ws)


def filled_with(x, identity):
    return jax.tree.map(
        lambda a, e: jnp.broadcast_to(jnp.asarray(e, a.dtype), a.shape), x, identity
    )


def entering(x, axes, combine, identity):
    before = start = filled_with(x, identity)
    total = x
    for axis in reversed(axes):
        length, place = (lax.axis_size(axis), lax.axis_index(axis))
        pieces = jax.tree.map(lambda part: lax.all_gather(part, axis), total)
        inside, total = (start, start)
        for k in range(length):
            passed = k < place
            total = combine(total, jax.tree.map(lambda part: part[k], pieces))
            inside = jax.tree.map(lambda new, old: jnp.where(passed, new, old), total, inside)
        before = combine(inside, before)
    return before


def from_behind(x, axis, by):
    length = lax.axis_size(axis)
    pairs = [(i, i + by) for i in range(length) if 0 <= i + by < length]
    return lax.ppermute(x, axis, pairs)


def rotate(vectors, positions):
    half_width = vectors.shape[-1] // 2
    frequency = rope_base ** (-jnp.arange(half_width, dtype=jnp.float32) / half_width)
    angles = positions.astype(jnp.float32)[:, None] * frequency
    cosine = jnp.cos(angles)[:, None, :]
    sine_part = jnp.sin(angles)[:, None, :]
    front_half = vectors[..., :half_width]
    back_half = vectors[..., half_width:]
    return jnp.concatenate(
        [front_half * cosine - back_half * sine_part, front_half * sine_part + back_half * cosine],
        axis=-1,
    )


def prepare(queries, key_rows, values, positions):
    row_count = queries.shape[0]
    rotated_query = rotate(
        queries.astype(jnp.float32).reshape(row_count, -1, KEY), positions
    ).astype(jnp.bfloat16)
    rotated_keys = (
        rotate(key_rows.astype(jnp.float32).reshape(row_count, -1, KEY), positions) * KEY ** (-0.5)
    ).astype(jnp.bfloat16)
    value_heads = values.reshape(row_count, -1, VAL)
    return (rotated_query, rotated_keys, value_heads)


def decay_logs(first_head, head_total, all_heads, seq_length):
    ratio = (first_head + jnp.arange(head_total)).astype(jnp.float32) / (all_heads - 1)
    return (jnp.log(0.05) + ratio * jnp.log(18.0)) / seq_length


def local_parts(queries, key_rows, values, log_decay):
    row_count = queries.shape[0]
    indices = jnp.arange(row_count, dtype=jnp.float32)
    offsets = indices[:, None] - indices[None, :]
    causal = offsets >= 0
    weight = jnp.where(
        causal[None], jnp.exp(log_decay[:, None, None] * jnp.where(causal, offsets, 0.0)[None]), 0.0
    )
    scores = (
        jnp.einsum("ihd,jhd->hij", queries, key_rows, preferred_element_type=jnp.float32) * weight
    ).astype(jnp.bfloat16)
    within = jnp.einsum("hij,jhe->ihe", scores, values, preferred_element_type=jnp.float32)
    trailing = jnp.exp(log_decay[None, :] * (row_count - 1.0 - indices)[:, None])
    weighted = (key_rows.astype(jnp.float32) * trailing[:, :, None]).astype(jnp.bfloat16)
    contribution = jnp.einsum("jhd,jhe->hde", weighted, values, preferred_element_type=jnp.float32)
    return (within, contribution)


def cross_part(queries, carry_state, log_decay):
    row_count = queries.shape[0]
    indices = jnp.arange(row_count, dtype=jnp.float32)
    leading = jnp.exp(log_decay[None, :] * (indices + 1.0)[:, None])
    return (
        jnp.einsum("ihd,hde->ihe", queries.astype(jnp.float32), carry_state) * leading[:, :, None]
    )


def retain_finish(raw, switch):
    average = jnp.mean(raw, axis=-1, keepdims=True)
    spread = jnp.mean(jnp.square(raw - average), axis=-1, keepdims=True)
    normalized = ((raw - average) * lax.rsqrt(spread + group_eps)).reshape(raw.shape[0], -1)
    return (normalized * jax.nn.silu(switch.astype(jnp.float32))).astype(jnp.bfloat16)


def convolve_branch(gated_input, before, tap_slice, gain_slice, shift_slice, switch):
    padded = jnp.concatenate([before, gated_input], axis=0)
    row_count = gated_input.shape[0]
    summed = jnp.zeros(gated_input.shape, jnp.float32)
    for tap_index in range(tap_slice.shape[0]):
        summed = (
            summed
            + padded[tap_index : tap_index + row_count].astype(jnp.float32) * tap_slice[tap_index]
        )
    grouped = summed.reshape(row_count, -1, GROUP)
    average = jnp.mean(grouped, axis=-1, keepdims=True)
    spread = jnp.mean(jnp.square(grouped - average), axis=-1, keepdims=True)
    normalized = ((grouped - average) * lax.rsqrt(spread + layer_eps)).reshape(row_count, -1)
    normalized = normalized * gain_slice + shift_slice
    return (jax.nn.silu(normalized) * jax.nn.silu(switch.astype(jnp.float32))).astype(jnp.bfloat16)


def contract(hidden, matrix):
    return lax.dot_general(
        hidden, matrix, (((1,), (1,)), ((), ())), preferred_element_type=jnp.float32
    )


def join_states(earlier, later):
    return (earlier[0] * later[0], later[0][:, None, None] * earlier[1] + later[1])


SP = ("sp_0", "sp_1", "sp_2")
SP_TP = ("sp_0", "sp_1", "sp_2", "tp")


def local_a(tokens, norm_gain, query_weight, key_weight, value_weight, retain_gate, unit_value, unit_gate, convolve_gate, retain_output, convolve_output):
    return tuple(gather_project(
        tokens, norm_gain.reshape(1, -1), query_weight, key_weight, value_weight, retain_gate,
        unit_value, unit_gate, convolve_gate, retain_output, convolve_output,
    ))


def local_b(p0, p1, p2, w3, filter_taps, layer_gain, layer_shift):
    head_groups = lax.axis_size("tp")
    chain_length = lax.axis_size(SP)
    head_rank = lax.axis_index("tp")
    chain_rank = lax.axis_index(SP)
    key_rows, values = p0[:, :512], p0[:, 512:]
    queries, glu_value, glu_switch = p1[:, :512], p1[:, 512:1024], p1[:, 1024:]
    retain_switch, convolve_switch = p2[:, :1024], p2[:, 1024:]
    w3 = w3.reshape(2048, 1536)
    row_count = 512
    local_heads = queries.shape[1] // KEY
    positions = chain_rank * row_count + jnp.arange(row_count, dtype=jnp.int32)
    rotated_query, rotated_keys, value_heads = prepare(queries, key_rows, values, positions)
    log_decay = decay_logs(
        head_rank * local_heads, local_heads, local_heads * head_groups, row_count * chain_length
    )
    within, contribution = local_parts(rotated_query, rotated_keys, value_heads, log_decay)
    totals = jnp.exp(log_decay * row_count)
    gated_input = (
        glu_value.astype(jnp.float32) * jax.nn.sigmoid(glu_switch.astype(jnp.float32))
    ).astype(jnp.bfloat16)
    channels = gated_input.shape[1]
    before = from_behind(gated_input[row_count - (KW - 1) :], SP, 1)
    prefix = entering(
        (totals, contribution),
        SP,
        join_states,
        (jnp.ones_like(totals), jnp.zeros_like(contribution)),
    )
    incoming = prefix[1]
    raw = within + cross_part(rotated_query, incoming, log_decay)
    retain_hidden = retain_finish(raw, retain_switch)
    tap_slice = lax.dynamic_slice_in_dim(filter_taps, head_rank * channels, channels, 1)
    gain_slice = lax.dynamic_slice_in_dim(layer_gain, head_rank * channels, channels, 0)
    shift_slice = lax.dynamic_slice_in_dim(layer_shift, head_rank * channels, channels, 0)
    convolve_hidden = convolve_branch(
        gated_input, before, tap_slice, gain_slice, shift_slice, convolve_switch
    )
    return lax.psum_scatter(
        contract(jnp.concatenate([retain_hidden, convolve_hidden], axis=1), w3).astype(
            jnp.bfloat16
        ),
        "tp",
        scatter_dimension=0,
        tiled=True,
    )


def solution(mesh):
    from jax.sharding import Mesh

    finer = Mesh(mesh.devices.reshape(4, 4, 2, mesh.shape["tp"]), ("sp_0", "sp_1", "sp_2", "tp"))
    weight = P("sp", "tp")
    rows = P(("sp", "tp"), None)
    first = jax.shard_map(
        local_a,
        mesh=mesh,
        in_specs=(rows, P()) + (weight,) * 9,
        out_specs=(weight,) * 3 + (P("sp", "tp"),),
        check_vma=False,
    )
    fine = P(SP, "tp")
    second = jax.shard_map(
        local_b,
        mesh=finer,
        in_specs=(fine,) * 3 + (fine,) + (P(),) * 3,
        out_specs=P(SP_TP, None),
        check_vma=False,
    )

    def run(tokens, norm_gain, qw, kw, vw, rg, uv, ug, cg, taps, lg, ls, ro, co):
        p0, p1, p2, w3 = first(tokens, norm_gain, qw, kw, vw, rg, uv, ug, cg, ro, co)
        return second(p0, p1, p2, w3, taps, lg, ls)

    return run
```

```python
import numpy as np

import jax
import jax.numpy as jnp
from jax import lax
from jax.experimental import pallas as pl
from jax.experimental.pallas import tpu as pltpu
from jax.sharding import PartitionSpec as P

MESH = pl.DeviceIdType.MESH
KEY = 256
VAL = 512
KW = 31
SEQ = 16384
HEADS = 8
rms_eps = 1e-06
group_eps = 1.0
layer_eps = 0.001
rope_base = 10000.0
HOPS = (0, 3, 1, 2)
BF = jnp.bfloat16
F32 = jnp.float32


def rotation_tables():
    frequency = rope_base ** (-np.arange(128, dtype=np.float64) / 128)
    fine = np.arange(512)[:, None] * frequency
    coarse = 512 * np.arange(32)[:, None] * frequency
    pair = lambda a: np.stack([np.cos(a), np.sin(a)], axis=1).astype(np.float32)
    return np.moveaxis(pair(fine), 1, 0), pair(coarse)


def silu(a):
    return a / (1.0 + jnp.exp(-a))


def body(
    tok,
    gain,
    wq,
    wk,
    wv,
    wrg,
    wuv,
    wug,
    wcg,
    wro,
    wco,
    taps,
    lgain,
    lshift,
    fine,
    coarse,
    out,
    W,
    N,
    tokv,
    gainv,
    tapv,
    lgainv,
    lshiftv,
    finev,
    coarsev,
    PV,
    ROT,
    WT,
    RK,
    RQ,
    CF,
    PS,
    PC,
    TB,
    TS,
    SZ,
    SB,
    SF,
    STS,
    STM,
    RAW,
    GP,
    HS,
    HR,
    CV,
    HID,
    OP,
    RA,
    RB,
    OUTV,
    lsem,
    wss,
    wrs,
    nss,
    nrs,
    sss,
    srs,
    rss,
    rrs,
    osem,
):
    sp = lax.axis_index("sp")
    x = lax.axis_index("tp")
    c = sp % 2
    y = (sp // 2) % 4
    z = sp // 8

    def coords(k1, k2, cc):
        ky = k1 * (1 - cc) + k2 * cc
        kz = k2 * (1 - cc) + k1 * cc
        return (z + kz) % 4, (y + ky) % 4

    def place(zz, yy):
        return ((zz * 4 + yy) * 2 + c, x)

    def device(k1, k2):
        return place(*coords(k1, k2, c))

    n1p, n1m, n2p, n2m = device(1, 0), device(3, 0), device(0, 1), device(0, 3)
    partner = ((z * 4 + y) * 2 + 1 - c, x)
    xp, xm = (sp, (x + 1) % 4), (sp, (x + 3) % 4)
    after, before = ((sp + 1) % 32, x), ((sp + 31) % 32, x)

    def block(g, k1, k2, lo=0, rows=64):
        zz, yy = coords(k1, k2, c)
        return W.at[g, zz, yy, c, pl.ds(lo, rows), :]

    def other(g, k1, k2):
        zz, yy = coords(k1, k2, 1 - c)
        return W.at[g, zz, yy, 1 - c]

    loads = []

    def load(src, dst):
        cp = pltpu.make_async_copy(src, dst, lsem.at[len(loads)])
        cp.start()
        loads.append(cp)

    mine = pl.ds(pl.multiple_of(x * 512, 512), 512)
    own = lambda g, a, b: W.at[g, z, y, c, :, pl.ds(a, b)]
    load(wk, own(0, 0, 512))
    load(wv, own(0, 512, 1024))
    load(tok, tokv)
    load(gain, gainv)
    load(wq, own(1, 0, 512))
    load(wuv, own(1, 512, 512))
    load(wug, own(1, 1024, 512))
    load(wrg, own(2, 0, 1024))
    load(wcg, own(2, 1024, 512))
    load(wro, own(3, 0, 1024))
    load(wco, own(3, 1024, 512))
    load(taps.at[:, mine], tapv)
    load(lgain.at[:, mine], lgainv)
    load(lshift.at[:, mine], lshiftv)
    load(fine, finev)
    load(coarse.at[sp], coarsev)

    greeted = (n1p, n1m, n2p, n2m, device(2, 0), device(0, 2), partner, xp, xm, after, before)
    barrier = pltpu.get_barrier_semaphore()
    for dev in greeted:
        pl.semaphore_signal(barrier, inc=1, device_id=dev, device_id_type=MESH)
    for cp in loads[:2]:
        cp.wait()
    pl.semaphore_wait(barrier, len(greeted))

    sends = []

    def remote(src, dst, ss, rs, dev):
        return pltpu.make_async_remote_copy(
            src_ref=src, dst_ref=dst, send_sem=ss, recv_sem=rs, device_id=dev, device_id_type=MESH
        )

    def send(src, dst, ss, rs, dev):
        cp = remote(src, dst, ss, rs, dev)
        cp.start()
        sends.append(cp)

    def arrived(ref, ss, rs):
        remote(ref, ref, ss, rs, partner).wait_recv()

    def wsend(ref, g, i, dev):
        send(ref, ref, wss.at[g, i], wrs.at[g, i], dev)

    def wwait(ref, g, i):
        arrived(ref, wss.at[g, i], wrs.at[g, i])

    def s1(g):
        wsend(block(g, 0, 0), g, 0, n1p)
        wsend(block(g, 0, 0), g, 1, n1m)

    def s2(g):
        wwait(block(g, 3, 0), g, 0)
        wsend(block(g, 3, 0, 0, 32), g, 2, n1p)
        wwait(block(g, 1, 0), g, 1)
        wsend(block(g, 1, 0, 32, 32), g, 3, n1m)

    def s3(g):
        for j in range(3):
            k = HOPS[j]
            wsend(block(g, k, 0), g, 4 + j, n2p)
            wsend(block(g, k, 0), g, 8 + j, n2m)
            wsend(block(g, k, 0), g, 20 + j, partner)

    def s3b(g):
        wwait(block(g, 2, 0, 0, 32), g, 2)
        wwait(block(g, 2, 0, 32, 32), g, 3)
        wsend(block(g, 2, 0), g, 7, n2p)
        wsend(block(g, 2, 0), g, 11, n2m)
        wsend(block(g, 2, 0), g, 23, partner)

    def s4(g, j):
        k = HOPS[j]
        wwait(block(g, k, 3), g, 4 + j)
        wsend(block(g, k, 3, 0, 32), g, 12 + j, n2p)
        wsend(block(g, k, 3), g, 24 + j, partner)
        wwait(block(g, k, 1), g, 8 + j)
        wsend(block(g, k, 1, 32, 32), g, 16 + j, n2m)
        wsend(block(g, k, 1), g, 28 + j, partner)

    def s5(g, j):
        k = HOPS[j]
        wwait(block(g, k, 2, 0, 32), g, 12 + j)
        wwait(block(g, k, 2, 32, 32), g, 16 + j)
        wsend(block(g, k, 2), g, 32 + j, partner)

    def s6(g):
        for j in range(4):
            for q, k2 in enumerate((0, 3, 1, 2)):
                wwait(other(g, HOPS[j], k2), g, 20 + 4 * q + j)

    def log_decay(h):
        ratio = (2 * x + h).astype(F32) * (1.0 / (HEADS - 1))
        return (float(np.log(0.05)) + ratio * float(np.log(18.0))) * (1.0 / SEQ)

    ld = [log_decay(0), log_decay(1)]
    ldc = log_decay(c)

    def power(e):
        return jnp.exp(jnp.full((1, 512), e, F32))

    def flag(cond):
        return jnp.where(cond, 1.0, 0.0).astype(F32)

    def loop(n, f):
        def step(i, carry):
            f(i)
            return carry

        lax.fori_loop(0, n, step, 0)

    def rows_of(i, n):
        return pl.ds(pl.multiple_of(i * n, n), n)

    def tables():
        cb, sb = coarsev[0:1, :], coarsev[1:2, :]

        def rot(i):
            r = rows_of(i, 128)
            cf, sf = finev[0, r, :], finev[1, r, :]
            ROT[0, r, :] = cf * cb - sf * sb
            ROT[1, r, :] = sf * cb + cf * sb

        loop(4, rot)

        def weight(i):
            r = rows_of(i, 64)
            t = lax.broadcasted_iota(jnp.int32, (64, 512), 0) + i * 64
            s = lax.broadcasted_iota(jnp.int32, (64, 512), 1)
            off = t - s
            offf = jnp.maximum(off, 0).astype(F32)
            for h in range(2):
                WT[h, r, :] = jnp.where(off >= 0, jnp.exp(ld[h] * offf), 0.0)

        loop(8, weight)

    def rotate(a, r):
        front, back = a[:, :128], a[:, 128:]
        cos, sin = ROT[0, r, :], ROT[1, r, :]
        return front * cos - back * sin, front * sin + back * cos

    def matmul(g, n):
        cols = pl.ds(pl.multiple_of(n * 256, 256), 256)
        w = W[g, :, :, :, :, cols].reshape(2048, 256)
        lhs = N[...].reshape(512, 2048)
        return jnp.dot(lhs, w, preferred_element_type=F32).astype(BF), cols

    def project(g, first, count):
        def step(i):
            res, cols = matmul(g, first + i)
            PV[g, :, cols] = res

        loop(count, step)

    def keys():
        for h in range(2):

            def step(i, h=h):
                r = rows_of(i, 128)
                front, back = rotate(PV[0, r, h * 256 : h * 256 + 256].astype(F32), r)
                RK[h, r, 0:128] = (front * 0.0625).astype(BF)
                RK[h, r, 128:256] = (back * 0.0625).astype(BF)

            loop(4, step)
            s = lax.broadcasted_iota(jnp.int32, (512, 1), 0).astype(F32)
            trailing = jnp.exp(ld[h] * (511.0 - s))
            weighted = (RK[h].astype(F32) * trailing).astype(BF)
            CF[h] = lax.dot_general(
                weighted,
                PV[0, :, 512 + h * 512 : 1024 + h * 512],
                (((0,), (0,)), ((), ())),
                preferred_element_type=F32,
            )
        PS[...] = CF[1 - c].astype(BF)
        send(PS, PC, sss.at[0], srs.at[0], partner)

    def state1():
        arrived(PC, sss.at[0], srs.at[0])
        d = power(ldc * 512.0)
        a = d * flag(c == 0) + flag(c == 1)
        b = d * flag(c == 1) + flag(c == 0)
        total = CF[c] * a + PC[...].astype(F32) * b
        TB[...] = total.astype(BF).reshape(4, 64, 512)
        TS[y] = TB[y]
        for k in (1, 3, 2):
            yy = (y + k) % 4
            send(TB.at[yy], TS.at[y], sss.at[k], srs.at[k], place(z, yy))

    def state2():
        for k in (1, 3, 2):
            arrived(TS.at[(y + 4 - k) % 4], sss.at[k], srs.at[k])
        total = TS[3].astype(F32)
        for yy in range(3):
            total += TS[yy].astype(F32) * power(ldc * (1024.0 * (3 - yy)))
        SZ[z] = total.astype(BF)
        for k in (1, 3, 2):
            send(SZ.at[z], SZ.at[z], sss.at[3 + k], srs.at[3 + k], place((z + k) % 4, y))

    def state3():
        for k in (1, 3, 2):
            arrived(SZ.at[(z + 4 - k) % 4], sss.at[3 + k], srs.at[3 + k])
        acc = jnp.zeros((64, 512), F32)
        for zz in range(3):
            e = jnp.maximum(z - 1 - zz, 0).astype(F32) * 4096.0
            acc += SZ[zz].astype(F32) * (power(ldc * e) * flag(zz < z))
        step = power(ldc * 1024.0)
        for yy in range(4):
            SB[yy] = acc.astype(BF)
            if yy < 3:
                acc = acc * step + TS[yy].astype(F32)
        SF[y] = SB[y]
        for k in (1, 3, 2):
            yy = (y + k) % 4
            send(SB.at[yy], SF.at[y], sss.at[6 + k], srs.at[6 + k], place(z, yy))

    def state4():
        for k in (1, 3, 2):
            arrived(SF.at[(y + 4 - k) % 4], sss.at[6 + k], srs.at[6 + k])
        d = power(ldc * 512.0)
        s = SF[...].reshape(256, 512).astype(F32)
        one, zero = flag(c == 1), flag(c == 0)
        STS[...] = (s * (d * zero + one) + CF[c] * zero).astype(BF)
        STM[c] = (s * (d * one + zero) + PC[...].astype(F32) * one).astype(BF)
        send(STS, STM.at[c], sss.at[10], srs.at[10], partner)

    def gate_input():
        def step(i):
            r = rows_of(i, 64)
            value = PV[1, r, 512:1024].astype(F32)
            switch = PV[1, r, 1024:1536].astype(F32)
            gated = (value / (1.0 + jnp.exp(-switch))).astype(BF).astype(F32)
            GP[pl.ds(pl.multiple_of(i * 64 + 32, 32), 64), :] = gated

        loop(8, step)
        HS[...] = GP[512:544, :].astype(BF)
        send(HS, HR, sss.at[11], srs.at[11], after)

    def scores():
        for h in range(2):

            def step(i, h=h):
                r = rows_of(i, 128)
                front, back = rotate(PV[1, r, h * 256 : h * 256 + 256].astype(F32), r)
                RQ[h, r, 0:128] = front.astype(BF)
                RQ[h, r, 128:256] = back.astype(BF)

            loop(4, step)

            def attend(i, h=h):
                r = rows_of(i, 256)
                sc = lax.dot_general(
                    RQ[h, r, :], RK[h], (((1,), (1,)), ((), ())), preferred_element_type=F32
                )
                sc = (sc * WT[h, r, :]).astype(BF)
                RAW[h, r, :] = jnp.dot(
                    sc, PV[0, :, 512 + h * 512 : 1024 + h * 512], preferred_element_type=F32
                )

            loop(2, attend)

    def convolve():
        arrived(HR, sss.at[11], srs.at[11])
        GP[0:32, :] = HR[...].astype(F32) * flag(sp > 0)

        def step(i):
            base = pl.multiple_of((i // 2) * 64, 64)
            cols = pl.ds(pl.multiple_of((i % 2) * 256, 256), 256)
            window = GP[pl.ds(base, 96), cols]
            acc = jnp.zeros((64, 256), F32)
            for q in range(8):
                shifted = window if q == 0 else pltpu.roll(window, 96 - q, axis=0)
                for k in range(5):
                    w = 8 * k + q - 2
                    if 0 <= w < KW:
                        acc += shifted[8 * k : 8 * k + 64] * tapv[w : w + 1, cols]
            CV[pl.ds(base, 64), cols] = acc

        loop(16, step)

        def norm(i):
            r = rows_of(i, 64)
            a = CV[r, :]
            a = a - jnp.mean(a, axis=-1, keepdims=True)
            spread = jnp.mean(a * a, axis=-1, keepdims=True)
            a = a * lax.rsqrt(spread + layer_eps) * lgainv[...] + lshiftv[...]
            CV[r, :] = silu(a)

        loop(8, norm)

    def finish():
        arrived(STM.at[1 - c], sss.at[10], srs.at[10])
        for h in range(2):

            def step(i, h=h):
                r = rows_of(i, 256)
                cross = jnp.dot(RQ[h, r, :], STM[h], preferred_element_type=F32)
                t = lax.broadcasted_iota(jnp.int32, (256, 1), 0) + i * 256
                raw = RAW[h, r, :] + cross * jnp.exp(ld[h] * (t + 1).astype(F32))
                raw = raw - jnp.mean(raw, axis=-1, keepdims=True)
                spread = jnp.mean(raw * raw, axis=-1, keepdims=True)
                RAW[h, r, :] = raw * lax.rsqrt(spread + group_eps)

            loop(2, step)

    def gates(h):
        def step(i):
            res, cols = matmul(2, h * 2 + i)
            g = silu(res.astype(F32))
            part = pl.ds(pl.multiple_of(i * 256, 256), 256)
            a = RAW[h, :, part] if h < 2 else CV[:, part]
            HID[:, cols] = (a * g).astype(BF)

        loop(2, step)

    def out_piece(zz):
        w = W[3, zz].reshape(512, 1536)
        for half in range(2):
            part = lax.dot_general(
                HID[...],
                w[half * 256 : half * 256 + 256],
                (((1,), (1,)), ((), ())),
                preferred_element_type=F32,
            )
            OP[zz, :, :, half * 256 : half * 256 + 256] = part.astype(BF).reshape(4, 128, 256)

    xl, xr, xf = (x + 3) % 4, (x + 1) % 4, (x + 2) % 4

    def reduce1(n):
        send(OP.at[n, xf, pl.ds(0, 64), :], RA.at[n, 0], rss.at[n, 0], rrs.at[n, 0], xp)
        send(OP.at[n, xf, pl.ds(64, 64), :], RA.at[n, 1], rss.at[n, 1], rrs.at[n, 1], xm)

    def reduce2(n):
        arrived(RA.at[n, 0], rss.at[n, 0], rrs.at[n, 0])
        OP[n, xr, 0:64, :] = (OP[n, xr, 0:64, :].astype(F32) + RA[n, 0].astype(F32)).astype(BF)
        send(OP.at[n, xr], RB.at[n, 0], rss.at[n, 2], rrs.at[n, 2], xp)
        arrived(RA.at[n, 1], rss.at[n, 1], rrs.at[n, 1])
        OP[n, xl, 64:128, :] = (OP[n, xl, 64:128, :].astype(F32) + RA[n, 1].astype(F32)).astype(BF)
        send(OP.at[n, xl], RB.at[n, 1], rss.at[n, 3], rrs.at[n, 3], xm)

    written = []

    def reduce3(n):
        arrived(RB.at[n, 0], rss.at[n, 2], rrs.at[n, 2])
        arrived(RB.at[n, 1], rss.at[n, 3], rrs.at[n, 3])
        total = OP[n, x].astype(F32) + RB[n, 0].astype(F32) + RB[n, 1].astype(F32)
        OUTV[n] = total.astype(BF)
        cp = pltpu.make_async_copy(OUTV.at[n], out.at[:, pl.ds(n * 512, 512)], osem.at[n])
        cp.start()
        written.append(cp)

    s1(0)
    loads[2].wait()
    loads[3].wait()

    def normalize(i):
        r = rows_of(i, 64)
        tk = tokv[r, :].astype(F32)
        scale = lax.rsqrt(jnp.mean(tk * tk, axis=-1, keepdims=True) + rms_eps)
        N[x, r, :] = (tk * scale * gainv[...]).astype(BF)

    loop(2, normalize)
    for cp in loads[4:]:
        cp.wait()
    s1(1)
    s2(0)
    send(N.at[x], N.at[x], nss.at[0], nrs.at[0], xp)
    send(N.at[x], N.at[x], nss.at[1], nrs.at[1], xm)

    def rows_on():
        arrived(N.at[xl], nss.at[0], nrs.at[0])
        left = N.at[xl, pl.ds(0, 64), :]
        send(left, left, nss.at[2], nrs.at[2], xp)
        arrived(N.at[xr], nss.at[1], nrs.at[1])
        right = N.at[xr, pl.ds(64, 64), :]
        send(right, right, nss.at[3], nrs.at[3], xm)

    def rows_in():
        arrived(N.at[xf, pl.ds(0, 64), :], nss.at[2], nrs.at[2])
        arrived(N.at[xf, pl.ds(64, 64), :], nss.at[3], nrs.at[3])

    tasks = {
        (0, 0): [rows_on, tables],
        (0, 5): [rows_in],
        (1, 0): [lambda: project(0, 0, 2)],
        (1, 1): [lambda: project(0, 2, 2)],
        (1, 2): [lambda: project(0, 4, 2)],
        (1, 3): [keys],
        (1, 4): [state1],
        (2, 0): [state2, lambda: project(1, 0, 2)],
        (2, 1): [lambda: project(1, 2, 2)],
        (2, 2): [lambda: project(1, 4, 2), gate_input],
        (2, 3): [state3],
        (2, 4): [scores],
        (2, 5): [state4],
        (3, 0): [convolve],
        (3, 1): [finish],
        (3, 2): [lambda: gates(0)],
        (3, 3): [lambda: gates(1)],
        (3, 4): [lambda: gates(2)],
    }

    def slot(g, k):
        for f in tasks.get((g, k), ()):
            f()

    for g in range(4):
        s3(g)
        if g + 2 < 4:
            s1(g + 2)
        s3b(g)
        if g + 1 < 4:
            s2(g + 1)
        slot(g, 0)
        for j in range(4):
            s4(g, j)
            slot(g, 1 + j)
        for j in range(4):
            s5(g, j)
        slot(g, 5)
        s6(g)

    out_piece(0)
    reduce1(0)
    out_piece(1)
    reduce1(1)
    reduce2(0)
    out_piece(2)
    reduce1(2)
    reduce2(1)
    out_piece(3)
    reduce1(3)
    reduce2(2)
    reduce2(3)
    for n in range(4):
        reduce3(n)
    for cp in written:
        cp.wait()
    for cp in sends:
        cp.wait_send()


def layer(tokens, gain, wq, wk, wv, wrg, wuv, wug, wcg, taps, lgain, lshift, wro, wco):
    any_spec = pl.BlockSpec(memory_space=pl.ANY)
    fine, coarse = rotation_tables()
    vm = pltpu.VMEM
    dma = pltpu.SemaphoreType.DMA
    row = lambda a: a.reshape(1, -1)
    return pl.pallas_call(
        body,
        out_shape=jax.ShapeDtypeStruct((128, 2048), BF),
        in_specs=[any_spec] * 16,
        out_specs=any_spec,
        scratch_shapes=[
            vm((4, 4, 4, 2, 64, 1536), BF),
            vm((4, 128, 2048), BF),
            vm((128, 2048), BF),
            vm((1, 2048), F32),
            vm((KW, 512), F32),
            vm((1, 512), F32),
            vm((1, 512), F32),
            vm((2, 512, 128), F32),
            vm((2, 128), F32),
            vm((2, 512, 1536), BF),
            vm((2, 512, 128), F32),
            vm((2, 512, 512), F32),
            vm((2, 512, 256), BF),
            vm((2, 512, 256), BF),
            vm((2, 256, 512), F32),
            vm((256, 512), BF),
            vm((256, 512), BF),
            vm((4, 64, 512), BF),
            vm((4, 64, 512), BF),
            vm((4, 64, 512), BF),
            vm((4, 64, 512), BF),
            vm((4, 64, 512), BF),
            vm((256, 512), BF),
            vm((2, 256, 512), BF),
            vm((2, 512, 512), F32),
            vm((544, 512), F32),
            vm((32, 512), BF),
            vm((32, 512), BF),
            vm((512, 512), F32),
            vm((512, 1536), BF),
            vm((4, 4, 128, 512), BF),
            vm((4, 2, 64, 512), BF),
            vm((4, 2, 128, 512), BF),
            vm((4, 128, 512), BF),
            dma((16,)),
            dma((4, 36)),
            dma((4, 36)),
            dma((4,)),
            dma((4,)),
            dma((12,)),
            dma((12,)),
            dma((4, 4)),
            dma((4, 4)),
            dma((4,)),
        ],
        compiler_params=pltpu.CompilerParams(
            collective_id=0, has_side_effects=True, vmem_limit_bytes=60 * 1024 * 1024
        ),
        name="layer",
    )(
        tokens, row(gain), wq, wk, wv, wrg, wuv, wug, wcg, wro, wco,
        taps, row(lgain), row(lshift), jnp.asarray(fine), jnp.asarray(coarse),
    )


def solution(mesh):
    weight = P("sp", "tp")
    rows = P(("sp", "tp"), None)
    return jax.shard_map(
        layer,
        mesh=mesh,
        in_specs=(rows, P()) + (weight,) * 7 + (P(),) * 3 + (weight,) * 2,
        out_specs=rows,
        check_vma=False,
    )
```
